32 devices in a mesh: sp: 4 (over z), fs: 4 (over y, x), tp: 2 (over core).
Axes of the slice: x: 2, y: 2, z: 4, core: 2. Of those that a mesh axis runs over, the one named last changes fastest.
Arguments:
- hidden_in: bfloat16 [8192, 2048], P(('fs', 'sp'), 'tp'), parts along dimension 0, may hold values from -6 to 48
- in_gain: float32 [2048], replicated, may hold values from 0.1 to 1.9
- w_query: bfloat16 [2048, 1024], P(None, 'tp'), may hold values from -0.29972302 to 0.29972302
- w_key: bfloat16 [2048, 1024], P(None, 'tp'), may hold values from -0.29972302 to 0.29972302
- w_value: bfloat16 [2048, 1024], P(None, 'tp'), may hold values from -0.125 to 0.125
- w_gate: bfloat16 [2048, 1024], P(None, 'tp'), may hold values from -0.125 to 0.125
- w_inner: bfloat16 [2048, 1024], P(None, 'tp'), may hold values from -0.125 to 0.125
- w_bvec: bfloat16 [2048, 512], P(None, 'tp'), may hold values from -0.125 to 0.125
- w_cvec: bfloat16 [2048, 512], P(None, 'tp'), may hold values from -0.125 to 0.125
- w_step: bfloat16 [2048, 16], P(None, 'tp'), may hold values from -0.125 to 0.125
- conv_inner: bfloat16 [4, 1024], P(None, 'tp'), may hold values from -3 to 3
- conv_bvec: bfloat16 [4, 512], P(None, 'tp'), may hold values from -3 to 3
- conv_cvec: bfloat16 [4, 512], P(None, 'tp'), may hold values from -3 to 3
- a_log: float32 [16], P('tp'), may hold values from -16 to 0
- decay_add: float32 [8192, 16], P(('fs', 'sp'), 'tp'), parts along dimension 0, may hold values from -1 to 0
- lambdas: float32 [4], P('tp'), may hold values from 0.3 to 0.8
- head_gain: float32 [256], replicated, may hold values from 0.1 to 1.9
- ssm_gain: float32 [1024], P('tp'), may hold values from 0.1 to 1.9
- out_attn: bfloat16 [1024, 2048], P('tp'), may hold values from -0.125 to 0.125
- out_ssm: bfloat16 [1024, 2048], P('tp'), may hold values from -0.125 to 0.125
Outputs:
- layer_out: bfloat16 [8192, 2048], P(('fs', 'sp', 'tp')), parts along dimension 0
The draws below stay inside these ranges and needn't reach their ends.
There are 4 independent parts, one for each index of `fs`. The reference program is written for one: setup_inputs(seed, part) draws one part's arguments, and reference() takes and returns one part's arrays. A program takes and returns all parts, laid end to end along the dimension named above; an argument that names none is the same for every part. Nothing has to cross between parts.
All inputs are finite; a program needn't handle non-finite values.
Results may differ from the reference program's by a relative error of at most 0.012.
The reference program's roundings to bfloat16 on the way (of `normed`, `attn_out` and `ssm_out`) count: a program that leaves them out, or rounds other values in their place, can miss the bound.
Values may be sent and summed in bfloat16 or wider, within the bound.
A program may use at most 128 MiB of HBM per device.

```python
import math
import jax
import jax.numpy as jnp
from jax import lax

D = 2048
ATTN_HEADS = 4
QK_DIM = 128
MIXER_HEADS = 16
SSM_P = 64
STATE = 128
GROUPS = 4
CONV_TAPS = 4
BLOCK = 128
SEQUENCE_LENGTH = 2048
ATTN_W = 1024
SSM_W = 1024
BC = 512


def drawn_columns(key):
    shared = jax.random.fold_in(key, 11)
    spread = 1.6 * (D * 10 // 17) ** (-0.5)
    return jax.random.truncated_normal(shared, -4.0, 4.0, (ATTN_W,), jnp.float32) * spread


def drawn_weight(key, salt):
    own_key = jax.random.fold_in(key, salt)
    spread = (D * 10 // 17) ** (-0.5)
    base = jax.random.truncated_normal(own_key, -4.0, 4.0, (D, ATTN_W), jnp.float32) * spread
    leading = (jnp.arange(D) < 8).astype(jnp.float32)[:, None]
    return base + leading * drawn_columns(key)[None, :]


def draw_w_query(key, part):
    return drawn_weight(key, 1).astype(jnp.bfloat16)


def draw_w_key(key, part):
    return drawn_weight(key, 2).astype(jnp.bfloat16)


def draw_hidden_in(key, part):
    base_key = jax.random.fold_in(key, 21)
    position_random_key = jax.random.fold_in(key, 22)
    size_key = jax.random.fold_in(key, 23)
    count = max(4, SEQUENCE_LENGTH // 512)
    base = jax.random.truncated_normal(base_key, -6.0, 6.0, (SEQUENCE_LENGTH, D), jnp.float32)
    strength = jax.random.uniform(size_key, (count,), jnp.float32, 8.0, 32.0)
    places = jax.random.randint(position_random_key, (count,), 0, SEQUENCE_LENGTH)
    hits = jnp.arange(SEQUENCE_LENGTH)[:, None] == places[None, :]
    level = jnp.max(jnp.where(hits, strength[None, :], 0.0), axis=1)
    planted = (level > 0.0)[:, None] & (jnp.arange(D) < 8)[None, :]
    return jnp.where(planted, level[:, None], base).astype(jnp.bfloat16)


def draw_a_log(key, part):
    order_key, slow_key, fast_key = jax.random.split(key, 3)
    head_order = jax.random.permutation(order_key, MIXER_HEADS)
    fast_heads = head_order < MIXER_HEADS // 2
    slow_rate = jax.random.uniform(slow_key, (MIXER_HEADS,), jnp.float32, 0.1, 0.4) / SEQUENCE_LENGTH
    fast_rate = jax.random.uniform(fast_key, (MIXER_HEADS,), jnp.float32, 0.015, 0.04)
    return jnp.log(jnp.where(fast_heads, fast_rate, slow_rate))


def draw_decay_add(key, part):
    rate_key, rough_key, position_random_key, depth_random_key = jax.random.split(key, 4)
    block_count = SEQUENCE_LENGTH // BLOCK
    block_rates = jnp.exp(jax.random.uniform(rate_key, (block_count, 1), jnp.float32, jnp.log(0.15), jnp.log(1.2))) / SEQUENCE_LENGTH
    roughness = jax.random.uniform(rough_key, (SEQUENCE_LENGTH, MIXER_HEADS), jnp.float32, 0.5, 1.5)
    steady_baseline = -jnp.repeat(block_rates, BLOCK, axis=0) * roughness
    spike_positions = jax.random.randint(position_random_key, (3,), 0, SEQUENCE_LENGTH)
    spike_depth = jnp.log(jax.random.uniform(depth_random_key, (3, MIXER_HEADS), jnp.float32, 0.5, 0.8))
    spike_rows = (jnp.arange(SEQUENCE_LENGTH)[:, None] == spike_positions[None, :]).astype(jnp.float32)
    return steady_baseline + jnp.dot(spike_rows, spike_depth, precision=jax.lax.Precision.HIGHEST)


def level_of(rng, extent, cuts, low, largest):
    loudness = 1.0
    for axis_at, shards_of in cuts:
        heights = jax.random.uniform(jax.random.fold_in(jax.random.fold_in(rng, 6), axis_at), (shards_of,), jnp.float32, low / len(cuts), largest / len(cuts))
        loudness = loudness * jnp.repeat(jnp.exp(heights), extent[axis_at] // shards_of).reshape((-1,) + (1,) * (len(extent) - 1 - axis_at))
    return loudness


def noise(key, extent, scale, most, cuts=(), held_as=jnp.bfloat16):
    entries = scale * jax.random.normal(key, extent, jnp.float32)
    if cuts:
        entries = entries * level_of(key, extent, cuts, -0.22, 0.18)
    return jnp.clip(entries, -most, most).astype(held_as)


def setup_inputs(seed: int = 0, part: int = 0) -> dict:
    streams_of = jax.random.split(jax.random.key(seed), 21)
    part_keys = jax.random.split(jax.random.fold_in(streams_of[20], part), 21)
    return {
        "hidden_in": draw_hidden_in(jax.random.fold_in(jax.random.fold_in(streams_of[20], part), 71), part),
        "in_gain": jnp.clip(1.0 + 0.18 * jax.random.normal(streams_of[1], (D,), jnp.float32), 0.1, 1.9),
        "w_query": draw_w_query(jax.random.fold_in(streams_of[20], 71), part),
        "w_key": draw_w_key(jax.random.fold_in(streams_of[20], 71), part),
        "w_value": noise(streams_of[4], (D, ATTN_W), D ** -0.5, 0.125, ((1, 2),)),
        "w_gate": noise(streams_of[5], (D, SSM_W), D ** -0.5, 0.125, ((1, 2),)),
        "w_inner": noise(streams_of[6], (D, SSM_W), D ** -0.5, 0.125, ((1, 2),)),
        "w_bvec": noise(streams_of[7], (D, BC), D ** -0.5, 0.125, ((1, 2),)),
        "w_cvec": noise(streams_of[8], (D, BC), D ** -0.5, 0.125, ((1, 2),)),
        "w_step": noise(streams_of[9], (D, MIXER_HEADS), D ** -0.5, 0.125, ((1, 2),)),
        "conv_inner": noise(streams_of[10], (CONV_TAPS, SSM_W), 0.5, 3.0, ((1, 2),)),
        "conv_bvec": noise(streams_of[11], (CONV_TAPS, BC), 0.5, 3.0, ((1, 2),)),
        "conv_cvec": noise(streams_of[12], (CONV_TAPS, BC), 0.5, 3.0, ((1, 2),)),
        "a_log": draw_a_log(jax.random.fold_in(streams_of[20], 71), part),
        "decay_add": draw_decay_add(jax.random.fold_in(jax.random.fold_in(streams_of[20], part), 71), part),
        "lambdas": jnp.clip(0.3 + 0.5 * jax.random.uniform(streams_of[15], (ATTN_HEADS,), jnp.float32) ** level_of(streams_of[15], (ATTN_HEADS,), ((0, 2),), -0.2, 0.2), 0.3, 0.8),
        "head_gain": jnp.clip(1.0 + 0.18 * jax.random.normal(streams_of[16], (2 * QK_DIM,), jnp.float32), 0.1, 1.9),
        "ssm_gain": jnp.clip(1.0 + 0.18 * jax.random.normal(streams_of[17], (SSM_W,), jnp.float32), 0.1, 1.9),
        "out_attn": noise(streams_of[18], (ATTN_W, D), (ATTN_W + SSM_W) ** -0.5, 0.125, ((0, 2),)),
        "out_ssm": noise(streams_of[19], (SSM_W, D), (ATTN_W + SSM_W) ** -0.5, 0.125, ((0, 2),)),
    }


EPS = 1e-06
NEG = -1e+30

def rms_rows(values, gain):
    return values * lax.rsqrt(lax.optimization_barrier(jnp.mean(values * values, axis=-1, keepdims=True)) + EPS) * gain

def stored(values):
    return lax.optimization_barrier(values.astype(jnp.bfloat16))

def reference(hidden_in, in_gain, w_query, w_key, w_value, w_gate, w_inner, w_bvec, w_cvec, w_step, conv_inner, conv_bvec, conv_cvec, a_log, decay_add, lambdas, head_gain, ssm_gain, out_attn, out_ssm):
    length = hidden_in.shape[0]
    normed = stored(rms_rows(hidden_in.astype(jnp.float32), in_gain))

    def project(weight):
        return stored(jnp.dot(normed, weight, preferred_element_type=jnp.float32))
    query = project(w_query).reshape(length, ATTN_HEADS, 2, QK_DIM)
    keys = project(w_key).reshape(length, ATTN_HEADS, 2, QK_DIM).astype(jnp.float32)
    values = project(w_value).reshape(length, ATTN_HEADS, 2 * QK_DIM).astype(jnp.float32)
    gate_z = project(w_gate)
    inner = project(w_inner)
    b_pre = project(w_bvec)
    c_pre = project(w_cvec)
    step_pre = project(w_step)
    scale = QK_DIM ** (-0.5)
    positions = jnp.arange(length).astype(jnp.int32)
    row_block = math.gcd(length, 512)

    def attend(start):
        query_rows = lax.dynamic_slice_in_dim(query, start, row_block, 0).astype(jnp.float32)
        scores = jnp.einsum('qhmd,khmd->qhmk', query_rows, keys) * scale
        query_pos = start + jnp.arange(row_block).astype(jnp.int32)
        visible = (positions[None, :] <= query_pos[:, None])[:, None, None, :]
        peak = lax.optimization_barrier(jnp.max(jnp.where(visible, scores, NEG), axis=-1, keepdims=True))
        weights = jnp.where(visible, jnp.exp(scores - peak), 0.0)
        totals = lax.optimization_barrier(jnp.sum(weights, axis=-1))
        mixed = jnp.einsum('qhmk,khe->qhme', stored(weights).astype(jnp.float32), values)
        first_map = mixed[:, :, 0] / totals[:, :, 0, None]
        second_map = mixed[:, :, 1] / totals[:, :, 1, None]
        differ = first_map - lambdas[None, :, None] * second_map
        return stored(rms_rows(differ, head_gain)).reshape(row_block, ATTN_W)
    starts = jnp.arange(0, length, row_block).astype(jnp.int32)
    attn_out = lax.map(attend, starts).reshape(length, ATTN_W)

    def convolve(pre, weight):
        padded = jnp.pad(pre.astype(jnp.float32), ((CONV_TAPS - 1, 0), (0, 0)))
        summed = padded[0:length] * weight[0].astype(jnp.float32)
        for offset in range(1, CONV_TAPS):
            summed = summed + padded[offset:offset + length] * weight[offset].astype(jnp.float32)
        return stored(jax.nn.silu(summed))
    per_group = MIXER_HEADS // GROUPS
    block_count = length // BLOCK
    inputs_x = convolve(inner, conv_inner).reshape(block_count, BLOCK, MIXER_HEADS, SSM_P)
    inputs_b = convolve(b_pre, conv_bvec).reshape(block_count, BLOCK, GROUPS, STATE)
    inputs_c = convolve(c_pre, conv_cvec).reshape(block_count, BLOCK, GROUPS, STATE)
    step_size = jax.nn.softplus(step_pre.astype(jnp.float32))
    log_decay = -jnp.exp(a_log)[None, :] * step_size + decay_add
    causal = jnp.tril(jnp.ones((BLOCK, BLOCK), dtype=bool))

    def block_step(state, items):
        block_x, block_b, block_c, block_size, block_decay = items
        running = jnp.cumsum(block_decay, axis=0)
        decay = jnp.exp(jnp.where(causal[:, :, None], running[:, None, :] - running[None, :, :], NEG))
        intersection = jnp.einsum('tgk,sgk->tsg', block_c.astype(jnp.float32), block_b.astype(jnp.float32))
        matrix = stored(jnp.repeat(intersection, per_group, axis=2) * decay * block_size[None, :, :])
        inside = jnp.einsum('tsh,shp->thp', matrix.astype(jnp.float32), block_x.astype(jnp.float32))
        heads_c = jnp.repeat(block_c, per_group, axis=1).astype(jnp.float32)
        carried = jnp.einsum('thk,hpk->thp', heads_c, state, precision=lax.Precision.HIGHEST) * jnp.exp(running)[:, :, None]
        to_end = jnp.exp(running[-1:] - running) * block_size
        weighted = stored(block_x.astype(jnp.float32) * to_end[:, :, None])
        heads_b = jnp.repeat(block_b, per_group, axis=1).astype(jnp.float32)
        fresh = jnp.einsum('shp,shk->hpk', weighted.astype(jnp.float32), heads_b)
        return (state * jnp.exp(running[-1])[:, None, None] + fresh, inside + carried)
    start_state = jnp.zeros((MIXER_HEADS, SSM_P, STATE), jnp.float32)
    items = (inputs_x, inputs_b, inputs_c, step_size.reshape(block_count, BLOCK, MIXER_HEADS), log_decay.reshape(block_count, BLOCK, MIXER_HEADS))
    final_state, outputs = lax.scan(block_step, start_state, items)
    gated = outputs.reshape(length, SSM_W) * jax.nn.silu(gate_z.astype(jnp.float32))
    grouped = rms_rows(gated.reshape(length, GROUPS, SSM_W // GROUPS), 1.0)
    ssm_out = stored(grouped.reshape(length, SSM_W) * ssm_gain)
    joined = jnp.dot(attn_out, out_attn, preferred_element_type=jnp.float32) + jnp.dot(ssm_out, out_ssm, preferred_element_type=jnp.float32)
    return joined.astype(jnp.bfloat16)
```

```python
import functools

import jax
import jax.numpy as jnp
from jax import lax
from jax.experimental import pallas as pl
from jax.experimental.pallas import tpu as pltpu
from jax.sharding import PartitionSpec as P

D = 2048
QK_DIM = 128
SSM_P = 64
STATE = 128
BLOCK = 128
ROW_TILE = 256


EPS = 1e-06
NEG = -1e30


def from_behind(x, axis, by, first=0):
    length = lax.axis_size(axis)
    pairs = [(i, i + by) for i in range(first, length) if 0 <= i + by < length]
    return lax.ppermute(x, axis, pairs)


def swap(x):
    return lax.ppermute(x, "tp", [(0, 1), (1, 0)])


def softmax_step(query, key, value, mask, state):
    scores = lax.dot_general(
        query, key, (((1,), (1,)), ((), ())), preferred_element_type=jnp.float32
    ) * (QK_DIM ** (-0.5))
    if mask is not None:
        scores = jnp.where(mask, scores, NEG)
    peak = jnp.max(scores, axis=1, keepdims=True)
    if state is not None:
        peak = jnp.maximum(peak, state[0])
    weights = jnp.exp(scores - peak)
    totals = jnp.sum(weights, axis=1, keepdims=True)
    accum = jnp.dot(weights.astype(jnp.bfloat16), value, preferred_element_type=jnp.float32)
    if state is not None:
        shrink = jnp.exp(state[0] - peak)
        totals = totals + state[1] * shrink
        accum = accum + state[2] * shrink
    return peak, totals, accum


def update_maps(query_ref, key_ref, value_ref, stats_ref, accum_ref, mask, fresh):
    width = value_ref.shape[1]
    lane = lax.broadcasted_iota(jnp.int32, stats_ref.shape, 1)
    stats = None if fresh else stats_ref[...]
    packed = jnp.zeros(stats_ref.shape, jnp.float32)
    for m in range(2):
        columns = slice(m * QK_DIM, (m + 1) * QK_DIM)
        state = None
        if not fresh:
            state = (
                stats[:, 2 * m : 2 * m + 1],
                stats[:, 2 * m + 1 : 2 * m + 2],
                accum_ref[:, m * width : (m + 1) * width],
            )
        peak, totals, accum = softmax_step(
            query_ref[:, columns], key_ref[:, columns], value_ref[...], mask, state
        )
        accum_ref[:, m * width : (m + 1) * width] = accum
        packed = jnp.where(lane == 2 * m, peak, packed)
        packed = jnp.where(lane == 2 * m + 1, totals, packed)
    stats_ref[...] = packed


def attend_first(pieces, place_ref, query_ref, *refs):
    kv_refs, (stats_ref, accum_ref) = refs[:-2], refs[-2:]
    row = lax.broadcasted_iota(jnp.int32, (query_ref.shape[0], kv_refs[0].shape[0]), 0)
    row = row + pl.program_id(1) * query_ref.shape[0]
    column = lax.broadcasted_iota(jnp.int32, row.shape, 1)
    update_maps(query_ref, kv_refs[0], kv_refs[1], stats_ref, accum_ref, column <= row, True)
    for s in range(1, pieces):

        @pl.when(place_ref[0] >= s)
        def _():
            update_maps(
                query_ref, kv_refs[2 * s], kv_refs[2 * s + 1], stats_ref, accum_ref, None, False
            )


def attend_last(
    piece, place_ref, lambda_ref, gain_ref, query_ref, key_ref, value_ref, stats_in, accum_in,
    out_ref, stats_ref, accum_ref,
):
    stats_ref[...] = stats_in[...]
    accum_ref[...] = accum_in[...]

    @pl.when(place_ref[0] >= piece)
    def _():
        update_maps(query_ref, key_ref, value_ref, stats_ref, accum_ref, None, False)

    width = value_ref.shape[1]
    stats = stats_ref[...]
    differ = accum_ref[:, :width] / stats[:, 1:2] - lambda_ref[pl.program_id(0)] * (
        accum_ref[:, width:] / stats[:, 3:4]
    )
    square = jnp.mean(differ * differ, axis=1, keepdims=True)
    out_ref[...] = (differ * lax.rsqrt(square + EPS) * gain_ref[...]).astype(jnp.bfloat16)


def attention(query, keys, values, lambdas, head_gain):
    rows, width = query.shape
    heads = lambdas.shape[0]
    wide = width // heads
    tile = min(ROW_TILE, rows)
    length = lax.axis_size("sp")
    place = lax.axis_index("sp").astype(jnp.int32).reshape(1)
    key_pieces, value_pieces = [keys], [values]
    for s in range(1, length):
        key_pieces.append(from_behind(key_pieces[-1], "sp", 1, s - 1))
        value_pieces.append(from_behind(value_pieces[-1], "sp", 1, s - 1))
    grid = (heads, rows // tile)
    smem = pl.BlockSpec(memory_space=pltpu.SMEM)
    by_rows = lambda cols: pl.BlockSpec((tile, cols), lambda h, r: (r, h))
    by_head = pl.BlockSpec((rows, wide), lambda h, r: (0, h))
    kv = [x for pair in zip(key_pieces[:-1], value_pieces[:-1]) for x in pair]
    flops = 2 * rows * rows * heads * 2 * (QK_DIM + wide)
    params = pltpu.CompilerParams(dimension_semantics=("arbitrary", "arbitrary"))
    stats, accum = pl.pallas_call(
        functools.partial(attend_first, length - 1),
        grid=grid,
        in_specs=[smem, by_rows(wide)] + [by_head] * len(kv),
        out_specs=[by_rows(128), by_rows(2 * wide)],
        out_shape=[
            jax.ShapeDtypeStruct((rows, heads * 128), jnp.float32),
            jax.ShapeDtypeStruct((rows, heads * 2 * wide), jnp.float32),
        ],
        compiler_params=params,
        cost_estimate=pl.CostEstimate(
            flops=flops * (length - 1), bytes_accessed=8 * rows * width, transcendentals=0
        ),
        name="attend_first",
    )(place, query, *kv)
    return pl.pallas_call(
        functools.partial(attend_last, length - 1),
        grid=grid,
        in_specs=[
            smem,
            smem,
            pl.BlockSpec((1, wide), lambda h, r: (0, 0)),
            by_rows(wide),
            by_head,
            by_head,
            by_rows(128),
            by_rows(2 * wide),
        ],
        out_specs=by_rows(wide),
        out_shape=jax.ShapeDtypeStruct((rows, width), jnp.bfloat16),
        scratch_shapes=[
            pltpu.VMEM((tile, 128), jnp.float32),
            pltpu.VMEM((tile, 2 * wide), jnp.float32),
        ],
        compiler_params=params,
        cost_estimate=pl.CostEstimate(
            flops=flops, bytes_accessed=12 * rows * width, transcendentals=0
        ),
        name="attend_last",
    )(place, lambdas, head_gain[None, :], query, key_pieces[-1], value_pieces[-1], stats, accum)


def per_device(
    hidden_in,
    in_gain,
    w_query,
    w_key,
    w_value,
    w_gate,
    w_inner,
    w_bvec,
    w_cvec,
    w_step,
    conv_inner,
    conv_bvec,
    conv_cvec,
    a_log,
    decay_add,
    lambdas,
    head_gain,
    ssm_gain,
    out_attn,
    out_ssm,
):
    rows_dev, half_width = hidden_in.shape
    other_half = swap(hidden_in)
    tp_index = lax.axis_index("tp")
    in_float = jnp.concatenate(
        [
            jnp.where(tp_index == 0, hidden_in, other_half),
            jnp.where(tp_index == 0, other_half, hidden_in),
        ],
        axis=1,
    ).astype(jnp.float32)
    squares = jnp.mean(in_float * in_float, axis=1, keepdims=True)
    whole = (in_float * lax.rsqrt(squares + EPS) * in_gain[None, :]).astype(jnp.bfloat16)
    swapped_attn, swapped_ssm = swap(out_attn), swap(out_ssm)
    weight_list = (w_key, w_value, w_query, w_gate, w_inner, w_bvec, w_cvec, w_step)
    keys, values, query, gate_z, inner, b_pre, c_pre, step_pre = [
        jnp.dot(whole, weight, preferred_element_type=jnp.float32).astype(jnp.bfloat16)
        for weight in weight_list
    ]
    attn_out = attention(query, keys, values, lambdas, head_gain)
    heads_ssm = a_log.shape[0]
    groups_local = b_pre.shape[1] // STATE
    per_group = heads_ssm // groups_local
    stacked = jnp.concatenate([inner, b_pre, c_pre], axis=1)
    taps = conv_inner.shape[0]
    earlier = from_behind(stacked[rows_dev - (taps - 1) :], "sp", 1)
    padded = jnp.concatenate([earlier, stacked], axis=0).astype(jnp.float32)
    conv_weight = jnp.concatenate([conv_inner, conv_bvec, conv_cvec], axis=1).astype(jnp.float32)
    summed = padded[0:rows_dev] * conv_weight[0]
    for offset in range(1, taps):
        summed = summed + padded[offset : offset + rows_dev] * conv_weight[offset]
    activated = jax.nn.silu(summed).astype(jnp.bfloat16)
    width_inner = inner.shape[1]
    width_vec = b_pre.shape[1]
    block_count = rows_dev // BLOCK
    inputs_x = activated[:, :width_inner].reshape(block_count, BLOCK, heads_ssm, SSM_P)
    inputs_b = activated[:, width_inner : width_inner + width_vec].reshape(
        block_count, BLOCK, groups_local, STATE
    )
    inputs_c = activated[:, width_inner + width_vec :].reshape(
        block_count, BLOCK, groups_local, STATE
    )
    step_size = jax.nn.softplus(step_pre.astype(jnp.float32))
    log_decay = -jnp.exp(a_log)[None, :] * step_size + decay_add
    size_major = step_size.reshape(block_count, BLOCK, heads_ssm).transpose(0, 2, 1)
    running = jnp.cumsum(
        log_decay.reshape(block_count, BLOCK, heads_ssm).transpose(0, 2, 1), axis=2
    )
    causal = jnp.tril(jnp.ones((BLOCK, BLOCK), dtype=bool))
    decay = jnp.exp(
        jnp.where(causal[None, None], running[:, :, :, None] - running[:, :, None, :], NEG)
    )
    intersection = jnp.einsum(
        "ntgk,nsgk->ngts", inputs_c, inputs_b, preferred_element_type=jnp.float32
    )
    matrix = (
        jnp.repeat(intersection, per_group, axis=1) * decay * size_major[:, :, None, :]
    ).astype(jnp.bfloat16)
    inside = jnp.einsum("nhts,nshp->nthp", matrix, inputs_x, preferred_element_type=jnp.float32)
    to_end = (jnp.exp(running[:, :, -1:] - running) * size_major).transpose(0, 2, 1)
    weighted = (inputs_x.astype(jnp.float32) * to_end[..., None]).astype(jnp.bfloat16)
    heads_b = jnp.repeat(inputs_b, per_group, axis=2)
    fresh = jnp.einsum("nshp,nshk->nhpk", weighted, heads_b, preferred_element_type=jnp.float32)
    block_totals = running[:, :, -1]

    def chain(state, items):
        fresh_block, total_block = items
        return (state * jnp.exp(total_block)[:, None, None] + fresh_block, state)

    local_end, local_enter = lax.scan(
        chain, jnp.zeros((heads_ssm, SSM_P, STATE), jnp.float32), (fresh, block_totals)
    )
    device_total = jnp.sum(block_totals, axis=0)
    sent_state = local_end.astype(jnp.bfloat16)
    my_index = lax.axis_index("sp")
    incoming = jnp.zeros_like(local_end)
    span = jnp.zeros_like(device_total)
    for by in range(1, lax.axis_size("sp")):
        state_by = from_behind(sent_state, "sp", by).astype(jnp.float32)
        incoming = incoming + jnp.where(my_index >= by, jnp.exp(span), 0.0)[:, None, None] * state_by
        span = span + from_behind(device_total, "sp", by)
    preceding = jnp.concatenate(
        [jnp.zeros((1, heads_ssm), jnp.float32), jnp.cumsum(block_totals, axis=0)[:-1]], axis=0
    )
    entering = local_enter + incoming[None] * jnp.exp(preceding)[:, :, None, None]
    heads_c = jnp.repeat(inputs_c, per_group, axis=2).astype(jnp.float32)
    carried = (
        jnp.einsum("nthk,nhpk->nthp", heads_c, entering, precision=lax.Precision.HIGHEST)
        * jnp.exp(running).transpose(0, 2, 1)[..., None]
    )
    ssm_y = (inside + carried).reshape(rows_dev, heads_ssm * SSM_P)
    gated = (ssm_y * jax.nn.silu(gate_z.astype(jnp.float32))).reshape(rows_dev, groups_local, -1)
    grouped = gated * lax.rsqrt(jnp.mean(gated * gated, axis=-1, keepdims=True) + EPS)
    ssm_out = (grouped.reshape(rows_dev, heads_ssm * SSM_P) * ssm_gain).astype(jnp.bfloat16)
    half = rows_dev // 2

    def own_and_other(array):
        own = lax.dynamic_slice_in_dim(array, tp_index * half, half, 0)
        other = lax.dynamic_slice_in_dim(array, (1 - tp_index) * half, half, 0)
        return own, swap(other)

    ssm_own, ssm_other = own_and_other(ssm_out)
    joined = jnp.dot(ssm_own, out_ssm, preferred_element_type=jnp.float32) + jnp.dot(
        ssm_other, swapped_ssm, preferred_element_type=jnp.float32
    )
    attn_own, attn_other = own_and_other(attn_out)
    joined = joined + jnp.dot(attn_own, out_attn, preferred_element_type=jnp.float32)
    joined = joined + jnp.dot(attn_other, swapped_attn, preferred_element_type=jnp.float32)
    return joined.astype(jnp.bfloat16)


def solution(mesh):
    in_specs = (
        P(("fs", "sp"), "tp"),
        P(),
        P(None, "tp"),
        P(None, "tp"),
        P(None, "tp"),
        P(None, "tp"),
        P(None, "tp"),
        P(None, "tp"),
        P(None, "tp"),
        P(None, "tp"),
        P(None, "tp"),
        P(None, "tp"),
        P(None, "tp"),
        P("tp"),
        P(("fs", "sp"), "tp"),
        P("tp"),
        P(),
        P("tp"),
        P("tp", None),
        P("tp", None),
    )
    out_specs = P(("fs", "sp", "tp"), None)
    return jax.shard_map(
        per_device, mesh=mesh, in_specs=in_specs, out_specs=out_specs, check_vma=False
    )
```

```python
import functools

import jax
import jax.numpy as jnp
from jax import lax
from jax.experimental import pallas as pl
from jax.experimental.pallas import tpu as pltpu
from jax.sharding import PartitionSpec as P

D = 2048
QK_DIM = 128
SSM_P = 64
STATE = 128
BLOCK = 128
ROW_TILE = 256


EPS = 1e-06
NEG = -1e30


def from_behind(x, axis, by, first=0):
    length = lax.axis_size(axis)
    pairs = [(i, i + by) for i in range(first, length) if 0 <= i + by < length]
    return lax.ppermute(x, axis, pairs)


def swap(x):
    return lax.ppermute(x, "tp", [(0, 1), (1, 0)])


def softmax_step(query, key, value, mask, state):
    scores = lax.dot_general(
        query, key, (((1,), (1,)), ((), ())), preferred_element_type=jnp.float32
    ) * (QK_DIM ** (-0.5))
    if mask is not None:
        scores = jnp.where(mask, scores, NEG)
    peak = jnp.max(scores, axis=1, keepdims=True)
    if state is not None:
        peak = jnp.maximum(peak, state[0])
    weights = jnp.exp(scores - peak)
    totals = jnp.sum(weights, axis=1, keepdims=True)
    accum = jnp.dot(weights.astype(jnp.bfloat16), value, preferred_element_type=jnp.float32)
    if state is not None:
        shrink = jnp.exp(state[0] - peak)
        totals = totals + state[1] * shrink
        accum = accum + state[2] * shrink
    return peak, totals, accum


def update_maps(query_ref, key_ref, value_ref, stats_ref, accum_ref, mask, fresh):
    width = value_ref.shape[1]
    lane = lax.broadcasted_iota(jnp.int32, stats_ref.shape, 1)
    stats = None if fresh else stats_ref[...]
    packed = jnp.zeros(stats_ref.shape, jnp.float32)
    for m in range(2):
        columns = slice(m * QK_DIM, (m + 1) * QK_DIM)
        state = None
        if not fresh:
            state = (
                stats[:, 2 * m : 2 * m + 1],
                stats[:, 2 * m + 1 : 2 * m + 2],
                accum_ref[:, m * width : (m + 1) * width],
            )
        peak, totals, accum = softmax_step(
            query_ref[:, columns], key_ref[:, columns], value_ref[...], mask, state
        )
        accum_ref[:, m * width : (m + 1) * width] = accum
        packed = jnp.where(lane == 2 * m, peak, packed)
        packed = jnp.where(lane == 2 * m + 1, totals, packed)
    stats_ref[...] = packed


def attend_first(pieces, place_ref, query_ref, *refs):
    kv_refs, (stats_ref, accum_ref) = refs[:-2], refs[-2:]
    row = lax.broadcasted_iota(jnp.int32, (query_ref.shape[0], kv_refs[0].shape[0]), 0)
    row = row + pl.program_id(1) * query_ref.shape[0]
    column = lax.broadcasted_iota(jnp.int32, row.shape, 1)
    update_maps(query_ref, kv_refs[0], kv_refs[1], stats_ref, accum_ref, column <= row, True)
    for s in range(1, pieces):

        @pl.when(place_ref[0] >= s)
        def _():
            update_maps(
                query_ref, kv_refs[2 * s], kv_refs[2 * s + 1], stats_ref, accum_ref, None, False
            )


def attend_last(
    piece, place_ref, lambda_ref, gain_ref, query_ref, key_ref, value_ref, stats_in, accum_in,
    out_ref, stats_ref, accum_ref,
):
    stats_ref[...] = stats_in[...]
    accum_ref[...] = accum_in[...]

    @pl.when(place_ref[0] >= piece)
    def _():
        update_maps(query_ref, key_ref, value_ref, stats_ref, accum_ref, None, False)

    width = value_ref.shape[1]
    stats = stats_ref[...]
    differ = accum_ref[:, :width] / stats[:, 1:2] - lambda_ref[pl.program_id(0)] * (
        accum_ref[:, width:] / stats[:, 3:4]
    )
    square = jnp.mean(differ * differ, axis=1, keepdims=True)
    out_ref[...] = (differ * lax.rsqrt(square + EPS) * gain_ref[...]).astype(jnp.bfloat16)


def attend_middle(
    piece, place_ref, query_ref, key_ref, value_ref, stats_in, accum_in, stats_ref, accum_ref
):
    stats_ref[...] = stats_in[...]
    accum_ref[...] = accum_in[...]

    @pl.when(place_ref[0] >= piece)
    def _():
        update_maps(query_ref, key_ref, value_ref, stats_ref, accum_ref, None, False)


def attention(query, key_pieces, value_pieces, lambdas, head_gain):
    rows, width = query.shape
    heads = lambdas.shape[0]
    wide = width // heads
    tile = min(ROW_TILE, rows)
    length = lax.axis_size("sp")
    place = lax.axis_index("sp").astype(jnp.int32).reshape(1)
    grid = (heads, rows // tile)
    smem = pl.BlockSpec(memory_space=pltpu.SMEM)
    by_rows = lambda cols: pl.BlockSpec((tile, cols), lambda h, r: (r, h))
    by_head = pl.BlockSpec((rows, wide), lambda h, r: (0, h))
    flops = 2 * rows * rows * heads * 2 * (QK_DIM + wide)
    params = pltpu.CompilerParams(dimension_semantics=("arbitrary", "arbitrary"))
    state_shape = [
        jax.ShapeDtypeStruct((rows, heads * 128), jnp.float32),
        jax.ShapeDtypeStruct((rows, heads * 2 * wide), jnp.float32),
    ]
    state_specs = [by_rows(128), by_rows(2 * wide)]
    early = min(2, length - 1)
    kv = [x for pair in zip(key_pieces[:early], value_pieces[:early]) for x in pair]
    stats, accum = pl.pallas_call(
        functools.partial(attend_first, early),
        grid=grid,
        in_specs=[smem, by_rows(wide)] + [by_head] * len(kv),
        out_specs=state_specs,
        out_shape=state_shape,
        compiler_params=params,
        cost_estimate=pl.CostEstimate(
            flops=flops * early, bytes_accessed=8 * rows * width, transcendentals=0
        ),
        name="attend_first",
    )(place, query, *kv)
    for piece in range(early, length - 1):
        stats, accum = pl.pallas_call(
            functools.partial(attend_middle, piece),
            grid=grid,
            in_specs=[smem, by_rows(wide), by_head, by_head] + state_specs,
            out_specs=state_specs,
            out_shape=state_shape,
            compiler_params=params,
            cost_estimate=pl.CostEstimate(
                flops=flops, bytes_accessed=16 * rows * width, transcendentals=0
            ),
            name="attend_middle",
        )(place, query, key_pieces[piece], value_pieces[piece], stats, accum)
    return pl.pallas_call(
        functools.partial(attend_last, length - 1),
        grid=grid,
        in_specs=[
            smem,
            smem,
            pl.BlockSpec((1, wide), lambda h, r: (0, 0)),
            by_rows(wide),
            by_head,
            by_head,
        ]
        + state_specs,
        out_specs=by_rows(wide),
        out_shape=jax.ShapeDtypeStruct((rows, width), jnp.bfloat16),
        scratch_shapes=[
            pltpu.VMEM((tile, 128), jnp.float32),
            pltpu.VMEM((tile, 2 * wide), jnp.float32),
        ],
        compiler_params=params,
        cost_estimate=pl.CostEstimate(
            flops=flops, bytes_accessed=12 * rows * width, transcendentals=0
        ),
        name="attend_last",
    )(place, lambdas, head_gain[None, :], query, key_pieces[-1], value_pieces[-1], stats, accum)


def add_products(base_ref, left_ref, left_weight, right_ref, right_weight, out_ref):
    total = base_ref[...] + jnp.dot(
        left_ref[...], left_weight[...], preferred_element_type=jnp.float32
    )
    total = total + jnp.dot(
        right_ref[...], right_weight[...], preferred_element_type=jnp.float32
    )
    out_ref[...] = total.astype(jnp.bfloat16)


def finish(base, left, left_weight, right, right_weight):
    rows, columns = base.shape
    depth = left.shape[1]
    tile = 512
    act = pl.BlockSpec((rows, depth), lambda j: (0, 0))
    weight = pl.BlockSpec((depth, tile), lambda j: (0, j))
    block = pl.BlockSpec((rows, tile), lambda j: (0, j))
    return pl.pallas_call(
        add_products,
        grid=(columns // tile,),
        in_specs=[block, act, weight, act, weight],
        out_specs=block,
        out_shape=jax.ShapeDtypeStruct((rows, columns), jnp.bfloat16),
        compiler_params=pltpu.CompilerParams(dimension_semantics=("arbitrary",)),
        cost_estimate=pl.CostEstimate(
            flops=4 * rows * depth * columns, bytes_accessed=8 * depth * columns, transcendentals=0
        ),
        name="finish",
    )(base, left, left_weight, right, right_weight)


def per_device(
    hidden_in,
    in_gain,
    w_query,
    w_key,
    w_value,
    w_gate,
    w_inner,
    w_bvec,
    w_cvec,
    w_step,
    conv_inner,
    conv_bvec,
    conv_cvec,
    a_log,
    decay_add,
    lambdas,
    head_gain,
    ssm_gain,
    out_attn,
    out_ssm,
):
    rows_dev, half_width = hidden_in.shape
    other_half = swap(hidden_in)
    tp_index = lax.axis_index("tp")
    in_float = jnp.concatenate(
        [
            jnp.where(tp_index == 0, hidden_in, other_half),
            jnp.where(tp_index == 0, other_half, hidden_in),
        ],
        axis=1,
    ).astype(jnp.float32)
    squares = jnp.mean(in_float * in_float, axis=1, keepdims=True)
    whole = (in_float * lax.rsqrt(squares + EPS) * in_gain[None, :]).astype(jnp.bfloat16)
    swapped_attn, swapped_ssm = swap(out_attn), swap(out_ssm)
    def project(rows_mat, weight):
        return jnp.dot(rows_mat, weight, preferred_element_type=jnp.float32).astype(jnp.bfloat16)

    keys = project(whole, w_key)
    values = project(whole, w_value)
    length = lax.axis_size("sp")
    key_pieces, value_pieces = [keys], [values]

    def hop():
        s = len(key_pieces)
        key_pieces.append(from_behind(key_pieces[-1], "sp", 1, s - 1))
        value_pieces.append(from_behind(value_pieces[-1], "sp", 1, s - 1))

    def arrived(*arrays):
        joint = lax.optimization_barrier((key_pieces[-1], value_pieces[-1]) + arrays)
        key_pieces[-1], value_pieces[-1] = joint[0], joint[1]
        return joint[2:]

    hop()
    whole, _, _ = lax.optimization_barrier((whole, keys, values))
    query, gate_z, inner, b_pre, c_pre, step_pre = [
        project(whole, weight)
        for weight in (w_query, w_gate, w_inner, w_bvec, w_cvec, w_step)
    ]
    heads_ssm = a_log.shape[0]
    groups_local = b_pre.shape[1] // STATE
    per_group = heads_ssm // groups_local
    stacked = jnp.concatenate([inner, b_pre, c_pre], axis=1)
    taps = conv_inner.shape[0]
    earlier = from_behind(stacked[rows_dev - (taps - 1) :], "sp", 1)
    padded = jnp.concatenate([earlier, stacked], axis=0).astype(jnp.float32)
    conv_weight = jnp.concatenate([conv_inner, conv_bvec, conv_cvec], axis=1).astype(jnp.float32)
    summed = padded[0:rows_dev] * conv_weight[0]
    for offset in range(1, taps):
        summed = summed + padded[offset : offset + rows_dev] * conv_weight[offset]
    activated = jax.nn.silu(summed).astype(jnp.bfloat16)
    width_inner = inner.shape[1]
    width_vec = b_pre.shape[1]
    block_count = rows_dev // BLOCK
    inputs_x = activated[:, :width_inner].reshape(block_count, BLOCK, heads_ssm, SSM_P)
    inputs_b = activated[:, width_inner : width_inner + width_vec].reshape(
        block_count, BLOCK, groups_local, STATE
    )
    inputs_c = activated[:, width_inner + width_vec :].reshape(
        block_count, BLOCK, groups_local, STATE
    )
    step_size = jax.nn.softplus(step_pre.astype(jnp.float32))
    log_decay = -jnp.exp(a_log)[None, :] * step_size + decay_add
    size_major = step_size.reshape(block_count, BLOCK, heads_ssm).transpose(0, 2, 1)
    running = jnp.cumsum(
        log_decay.reshape(block_count, BLOCK, heads_ssm).transpose(0, 2, 1), axis=2
    )
    causal = jnp.tril(jnp.ones((BLOCK, BLOCK), dtype=bool))
    decay = jnp.exp(
        jnp.where(causal[None, None], running[:, :, :, None] - running[:, :, None, :], NEG)
    )
    intersection = jnp.einsum(
        "ntgk,nsgk->ngts", inputs_c, inputs_b, preferred_element_type=jnp.float32
    )
    matrix = (
        jnp.repeat(intersection, per_group, axis=1) * decay * size_major[:, :, None, :]
    ).astype(jnp.bfloat16)
    inside = jnp.einsum("nhts,nshp->nthp", matrix, inputs_x, preferred_element_type=jnp.float32)
    to_end = (jnp.exp(running[:, :, -1:] - running) * size_major).transpose(0, 2, 1)
    weighted = (inputs_x.astype(jnp.float32) * to_end[..., None]).astype(jnp.bfloat16)
    heads_b = jnp.repeat(inputs_b, per_group, axis=2)
    fresh = jnp.einsum("nshp,nshk->nhpk", weighted, heads_b, preferred_element_type=jnp.float32)
    block_totals = running[:, :, -1]

    def chain(state, items):
        fresh_block, total_block = items
        return (state * jnp.exp(total_block)[:, None, None] + fresh_block, state)

    local_end, local_enter = lax.scan(
        chain, jnp.zeros((heads_ssm, SSM_P, STATE), jnp.float32), (fresh, block_totals)
    )
    device_total = jnp.sum(block_totals, axis=0)
    high = device_total.astype(jnp.bfloat16)
    rest = device_total - high.astype(jnp.float32)
    middle = rest.astype(jnp.bfloat16)
    low = (rest - middle.astype(jnp.float32)).astype(jnp.bfloat16)
    parts = jnp.stack([high, middle, low] + [jnp.zeros_like(high)] * 13, axis=1)
    packed = jnp.concatenate(
        [
            local_end.astype(jnp.bfloat16),
            jnp.broadcast_to(parts[:, :, None], (heads_ssm, 16, STATE)),
        ],
        axis=1,
    )
    my_index = lax.axis_index("sp")
    incoming = jnp.zeros_like(local_end)
    span = jnp.zeros_like(device_total)
    (packed,) = arrived(packed)
    came = [from_behind(packed, "sp", by) for by in range(1, length)]
    for s in range(2, length):
        hop()
        if s == 2:
            came = list(arrived(*came))
    for by in range(1, length):
        state_by = came[by - 1].astype(jnp.float32)
        incoming = (
            incoming
            + jnp.where(my_index >= by, jnp.exp(span), 0.0)[:, None, None] * state_by[:, :SSM_P]
        )
        span = span + jnp.sum(state_by[:, SSM_P : SSM_P + 3, 0], axis=1)
    preceding = jnp.concatenate(
        [jnp.zeros((1, heads_ssm), jnp.float32), jnp.cumsum(block_totals, axis=0)[:-1]], axis=0
    )
    entering = local_enter + incoming[None] * jnp.exp(preceding)[:, :, None, None]
    heads_c = jnp.repeat(inputs_c, per_group, axis=2).astype(jnp.float32)
    carried = (
        jnp.einsum("nthk,nhpk->nthp", heads_c, entering, precision=lax.Precision.HIGHEST)
        * jnp.exp(running).transpose(0, 2, 1)[..., None]
    )
    ssm_y = (inside + carried).reshape(rows_dev, heads_ssm * SSM_P)
    gated = (ssm_y * jax.nn.silu(gate_z.astype(jnp.float32))).reshape(rows_dev, groups_local, -1)
    grouped = gated * lax.rsqrt(jnp.mean(gated * gated, axis=-1, keepdims=True) + EPS)
    ssm_out = (grouped.reshape(rows_dev, heads_ssm * SSM_P) * ssm_gain).astype(jnp.bfloat16)
    half = rows_dev // 2

    def own_and_other(array):
        own = lax.dynamic_slice_in_dim(array, tp_index * half, half, 0)
        other = lax.dynamic_slice_in_dim(array, (1 - tp_index) * half, half, 0)
        return own, swap(other)

    ssm_own, ssm_other = own_and_other(ssm_out)
    joined = jnp.dot(ssm_own, out_ssm, preferred_element_type=jnp.float32) + jnp.dot(
        ssm_other, swapped_ssm, preferred_element_type=jnp.float32
    )
    attn_out = attention(query, key_pieces, value_pieces, lambdas, head_gain)
    attn_own, attn_other = own_and_other(attn_out)
    return finish(joined, attn_own, out_attn, attn_other, swapped_attn)


def solution(mesh):
    in_specs = (
        P(("fs", "sp"), "tp"),
        P(),
        P(None, "tp"),
        P(None, "tp"),
        P(None, "tp"),
        P(None, "tp"),
        P(None, "tp"),
        P(None, "tp"),
        P(None, "tp"),
        P(None, "tp"),
        P(None, "tp"),
        P(None, "tp"),
        P(None, "tp"),
        P("tp"),
        P(("fs", "sp"), "tp"),
        P("tp"),
        P(),
        P("tp"),
        P("tp", None),
        P("tp", None),
    )
    out_specs = P(("fs", "sp", "tp"), None)
    return jax.shard_map(
        per_device, mesh=mesh, in_specs=in_specs, out_specs=out_specs, check_vma=False
    )
```

```python
import functools

import jax
import jax.numpy as jnp
from jax import lax
from jax.experimental import pallas as pl
from jax.experimental.pallas import tpu as pltpu
from jax.sharding import PartitionSpec as P


QK_DIM = 128
SSM_P = 64
STATE = 128
BLOCK = 128
ROW_TILE = 256


EPS = 1e-06
NEG = -1e30


def from_behind(x, axis, by, first=0):
    length = lax.axis_size(axis)
    pairs = [(i, i + by) for i in range(first, length) if 0 <= i + by < length]
    return lax.ppermute(x, axis, pairs)


def swap(x):
    return lax.ppermute(x, "tp", [(0, 1), (1, 0)])


def softmax_step(query, key, value, mask, state):
    scores = lax.dot_general(
        query, key, (((1,), (1,)), ((), ())), preferred_element_type=jnp.float32
    ) * (QK_DIM ** (-0.5))
    if mask is not None:
        scores = jnp.where(mask, scores, NEG)
    peak = jnp.max(scores, axis=1, keepdims=True)
    if state is not None:
        peak = jnp.maximum(peak, state[0])
    weights = jnp.exp(scores - peak)
    totals = jnp.sum(weights, axis=1, keepdims=True)
    accum = jnp.dot(weights.astype(jnp.bfloat16), value, preferred_element_type=jnp.float32)
    if state is not None:
        shrink = jnp.exp(state[0] - peak)
        totals = totals + state[1] * shrink
        accum = accum + state[2] * shrink
    return peak, totals, accum


def update_maps(query_ref, key_ref, value_ref, stats_ref, accum_ref, mask, fresh):
    width = value_ref.shape[1]
    lane = lax.broadcasted_iota(jnp.int32, stats_ref.shape, 1)
    stats = None if fresh else stats_ref[...]
    packed = jnp.zeros(stats_ref.shape, jnp.float32)
    for m in range(2):
        columns = slice(m * QK_DIM, (m + 1) * QK_DIM)
        state = None
        if not fresh:
            state = (
                stats[:, 2 * m : 2 * m + 1],
                stats[:, 2 * m + 1 : 2 * m + 2],
                accum_ref[:, m * width : (m + 1) * width],
            )
        peak, totals, accum = softmax_step(
            query_ref[:, columns], key_ref[:, columns], value_ref[...], mask, state
        )
        accum_ref[:, m * width : (m + 1) * width] = accum
        packed = jnp.where(lane == 2 * m, peak, packed)
        packed = jnp.where(lane == 2 * m + 1, totals, packed)
    stats_ref[...] = packed


def attend_first(pieces, place_ref, query_ref, *refs):
    kv_refs, (stats_ref, accum_ref) = refs[:-2], refs[-2:]
    row = lax.broadcasted_iota(jnp.int32, (query_ref.shape[0], kv_refs[0].shape[0]), 0)
    row = row + pl.program_id(1) * query_ref.shape[0]
    column = lax.broadcasted_iota(jnp.int32, row.shape, 1)
    update_maps(query_ref, kv_refs[0], kv_refs[1], stats_ref, accum_ref, column <= row, True)
    for s in range(1, pieces):

        @pl.when(place_ref[0] >= s)
        def _():
            update_maps(
                query_ref, kv_refs[2 * s], kv_refs[2 * s + 1], stats_ref, accum_ref, None, False
            )


def attend_last(
    piece, place_ref, lambda_ref, gain_ref, query_ref, key_ref, value_ref, stats_in, accum_in,
    out_ref, stats_ref, accum_ref,
):
    stats_ref[...] = stats_in[...]
    accum_ref[...] = accum_in[...]

    @pl.when(place_ref[0] >= piece)
    def _():
        update_maps(query_ref, key_ref, value_ref, stats_ref, accum_ref, None, False)

    width = value_ref.shape[1]
    stats = stats_ref[...]
    differ = accum_ref[:, :width] / stats[:, 1:2] - lambda_ref[pl.program_id(0)] * (
        accum_ref[:, width:] / stats[:, 3:4]
    )
    square = jnp.mean(differ * differ, axis=1, keepdims=True)
    out_ref[...] = (differ * lax.rsqrt(square + EPS) * gain_ref[...]).astype(jnp.bfloat16)


def attend_middle(
    piece, place_ref, query_ref, key_ref, value_ref, stats_in, accum_in, stats_ref, accum_ref
):
    stats_ref[...] = stats_in[...]
    accum_ref[...] = accum_in[...]

    @pl.when(place_ref[0] >= piece)
    def _():
        update_maps(query_ref, key_ref, value_ref, stats_ref, accum_ref, None, False)


def attention(query, key_pieces, value_pieces, lambdas, head_gain):
    rows, width = query.shape
    heads = lambdas.shape[0]
    wide = width // heads
    tile = min(ROW_TILE, rows)
    length = lax.axis_size("sp")
    place = lax.axis_index("sp").astype(jnp.int32).reshape(1)
    grid = (heads, rows // tile)
    smem = pl.BlockSpec(memory_space=pltpu.SMEM)
    by_rows = lambda cols: pl.BlockSpec((tile, cols), lambda h, r: (r, h))
    by_head = pl.BlockSpec((rows, wide), lambda h, r: (0, h))
    flops = 2 * rows * rows * heads * 2 * (QK_DIM + wide)
    params = pltpu.CompilerParams(dimension_semantics=("arbitrary", "arbitrary"))
    state_shape = [
        jax.ShapeDtypeStruct((rows, heads * 128), jnp.float32),
        jax.ShapeDtypeStruct((rows, heads * 2 * wide), jnp.float32),
    ]
    state_specs = [by_rows(128), by_rows(2 * wide)]
    early = min(2, length - 1)
    kv = [x for pair in zip(key_pieces[:early], value_pieces[:early]) for x in pair]
    stats, accum = pl.pallas_call(
        functools.partial(attend_first, early),
        grid=grid,
        in_specs=[smem, by_rows(wide)] + [by_head] * len(kv),
        out_specs=state_specs,
        out_shape=state_shape,
        compiler_params=params,
        cost_estimate=pl.CostEstimate(
            flops=flops * early, bytes_accessed=8 * rows * width, transcendentals=0
        ),
        name="attend_first",
    )(place, query, *kv)
    for piece in range(early, length - 1):
        stats, accum = pl.pallas_call(
            functools.partial(attend_middle, piece),
            grid=grid,
            in_specs=[smem, by_rows(wide), by_head, by_head] + state_specs,
            out_specs=state_specs,
            out_shape=state_shape,
            compiler_params=params,
            cost_estimate=pl.CostEstimate(
                flops=flops, bytes_accessed=16 * rows * width, transcendentals=0
            ),
            name="attend_middle",
        )(place, query, key_pieces[piece], value_pieces[piece], stats, accum)
    stats = yield stats
    yield pl.pallas_call(
        functools.partial(attend_last, length - 1),
        grid=grid,
        in_specs=[
            smem,
            smem,
            pl.BlockSpec((1, wide), lambda h, r: (0, 0)),
            by_rows(wide),
            by_head,
            by_head,
        ]
        + state_specs,
        out_specs=by_rows(wide),
        out_shape=jax.ShapeDtypeStruct((rows, width), jnp.bfloat16),
        scratch_shapes=[
            pltpu.VMEM((tile, 128), jnp.float32),
            pltpu.VMEM((tile, 2 * wide), jnp.float32),
        ],
        compiler_params=params,
        cost_estimate=pl.CostEstimate(
            flops=flops, bytes_accessed=12 * rows * width, transcendentals=0
        ),
        name="attend_last",
    )(place, lambdas, head_gain[None, :], query, key_pieces[-1], value_pieces[-1], stats, accum)


def per_device(
    hidden_in,
    in_gain,
    w_query,
    w_key,
    w_value,
    w_gate,
    w_inner,
    w_bvec,
    w_cvec,
    w_step,
    conv_inner,
    conv_bvec,
    conv_cvec,
    a_log,
    decay_add,
    lambdas,
    head_gain,
    ssm_gain,
    out_attn,
    out_ssm,
):
    rows_dev, _ = hidden_in.shape
    other_half = swap(hidden_in)
    tp_index = lax.axis_index("tp")
    in_float = jnp.concatenate(
        [
            jnp.where(tp_index == 0, hidden_in, other_half),
            jnp.where(tp_index == 0, other_half, hidden_in),
        ],
        axis=1,
    ).astype(jnp.float32)
    squares = jnp.mean(in_float * in_float, axis=1, keepdims=True)
    whole = (in_float * lax.rsqrt(squares + EPS) * in_gain[None, :]).astype(jnp.bfloat16)
    swapped_attn, swapped_ssm = swap(out_attn), swap(out_ssm)

    def project(rows_mat, weight):
        return jnp.dot(rows_mat, weight, preferred_element_type=jnp.float32).astype(jnp.bfloat16)

    inner, b_pre, c_pre = [project(whole, weight) for weight in (w_inner, w_bvec, w_cvec)]
    stacked = jnp.concatenate([inner, b_pre, c_pre], axis=1)
    taps = conv_inner.shape[0]
    earlier = from_behind(stacked[rows_dev - (taps - 1) :], "sp", 1)
    whole, _ = lax.optimization_barrier((whole, stacked))
    keys = project(whole, w_key)
    values = project(whole, w_value)
    length = lax.axis_size("sp")
    keys, earlier = lax.optimization_barrier((keys, earlier))
    key_pieces, value_pieces = [keys], [values]

    def hop():
        s = len(key_pieces)
        key_pieces.append(from_behind(key_pieces[-1], "sp", 1, s - 1))
        value_pieces.append(from_behind(value_pieces[-1], "sp", 1, s - 1))

    def arrived(*arrays):
        joint = lax.optimization_barrier((key_pieces[-1], value_pieces[-1]) + arrays)
        key_pieces[-1], value_pieces[-1] = joint[0], joint[1]
        return joint[2:]

    hop()
    whole, _, _ = lax.optimization_barrier((whole, keys, values))
    query, gate_z, step_pre = [project(whole, weight) for weight in (w_query, w_gate, w_step)]
    heads_ssm = a_log.shape[0]
    groups_local = b_pre.shape[1] // STATE
    per_group = heads_ssm // groups_local
    padded = jnp.concatenate([earlier, stacked], axis=0).astype(jnp.float32)
    conv_weight = jnp.concatenate([conv_inner, conv_bvec, conv_cvec], axis=1).astype(jnp.float32)
    summed = padded[0:rows_dev] * conv_weight[0]
    for offset in range(1, taps):
        summed = summed + padded[offset : offset + rows_dev] * conv_weight[offset]
    activated = jax.nn.silu(summed).astype(jnp.bfloat16)
    width_inner = inner.shape[1]
    width_vec = b_pre.shape[1]
    block_count = rows_dev // BLOCK
    inputs_x = activated[:, :width_inner].reshape(block_count, BLOCK, heads_ssm, SSM_P)
    inputs_b = activated[:, width_inner : width_inner + width_vec].reshape(
        block_count, BLOCK, groups_local, STATE
    )
    inputs_c = activated[:, width_inner + width_vec :].reshape(
        block_count, BLOCK, groups_local, STATE
    )
    step_size = jax.nn.softplus(step_pre.astype(jnp.float32))
    log_decay = -jnp.exp(a_log)[None, :] * step_size + decay_add
    size_major = step_size.reshape(block_count, BLOCK, heads_ssm).transpose(0, 2, 1)
    running = jnp.cumsum(
        log_decay.reshape(block_count, BLOCK, heads_ssm).transpose(0, 2, 1), axis=2
    )
    causal = jnp.tril(jnp.ones((BLOCK, BLOCK), dtype=bool))
    decay = jnp.exp(
        jnp.where(causal[None, None], running[:, :, :, None] - running[:, :, None, :], NEG)
    )
    intersection = jnp.einsum(
        "ntgk,nsgk->ngts", inputs_c, inputs_b, preferred_element_type=jnp.float32
    )
    matrix = (
        jnp.repeat(intersection, per_group, axis=1) * decay * size_major[:, :, None, :]
    ).astype(jnp.bfloat16)
    inside = jnp.einsum("nhts,nshp->nthp", matrix, inputs_x, preferred_element_type=jnp.float32)
    to_end = (jnp.exp(running[:, :, -1:] - running) * size_major).transpose(0, 2, 1)
    weighted = (inputs_x.astype(jnp.float32) * to_end[..., None]).astype(jnp.bfloat16)
    heads_b = jnp.repeat(inputs_b, per_group, axis=2)
    fresh = jnp.einsum("nshp,nshk->nhpk", weighted, heads_b, preferred_element_type=jnp.float32)
    block_totals = running[:, :, -1]

    def chain(state, items):
        fresh_block, total_block = items
        return (state * jnp.exp(total_block)[:, None, None] + fresh_block, state)

    local_end, local_enter = lax.scan(
        chain, jnp.zeros((heads_ssm, SSM_P, STATE), jnp.float32), (fresh, block_totals)
    )
    device_total = jnp.sum(block_totals, axis=0)
    high = device_total.astype(jnp.bfloat16)
    rest = device_total - high.astype(jnp.float32)
    middle = rest.astype(jnp.bfloat16)
    low = (rest - middle.astype(jnp.float32)).astype(jnp.bfloat16)
    parts = jnp.stack([high, middle, low] + [jnp.zeros_like(high)] * 13, axis=1)
    packed = jnp.concatenate(
        [
            local_end.astype(jnp.bfloat16),
            jnp.broadcast_to(parts[:, :, None], (heads_ssm, 16, STATE)),
        ],
        axis=1,
    )
    my_index = lax.axis_index("sp")
    incoming = jnp.zeros_like(local_end)
    span = jnp.zeros_like(device_total)
    (packed,) = arrived(packed)
    came = [from_behind(packed, "sp", by) for by in range(1, length)]
    for _ in range(2, length):
        hop()
    attending = attention(query, key_pieces, value_pieces, lambdas, head_gain)
    stats, *came = lax.optimization_barrier((next(attending), *came))
    for by in range(1, length):
        state_by = came[by - 1].astype(jnp.float32)
        incoming = (
            incoming
            + jnp.where(my_index >= by, jnp.exp(span), 0.0)[:, None, None] * state_by[:, :SSM_P]
        )
        span = span + jnp.sum(state_by[:, SSM_P : SSM_P + 3, 0], axis=1)
    preceding = jnp.concatenate(
        [jnp.zeros((1, heads_ssm), jnp.float32), jnp.cumsum(block_totals, axis=0)[:-1]], axis=0
    )
    entering = local_enter + incoming[None] * jnp.exp(preceding)[:, :, None, None]
    heads_c = jnp.repeat(inputs_c, per_group, axis=2).astype(jnp.float32)
    carried = (
        jnp.einsum("nthk,nhpk->nthp", heads_c, entering, precision=lax.Precision.HIGHEST)
        * jnp.exp(running).transpose(0, 2, 1)[..., None]
    )
    ssm_y = (inside + carried).reshape(rows_dev, heads_ssm * SSM_P)
    gated = (ssm_y * jax.nn.silu(gate_z.astype(jnp.float32))).reshape(rows_dev, groups_local, -1)
    grouped = gated * lax.rsqrt(jnp.mean(gated * gated, axis=-1, keepdims=True) + EPS)
    ssm_out = (grouped.reshape(rows_dev, heads_ssm * SSM_P) * ssm_gain).astype(jnp.bfloat16)
    half = rows_dev // 2

    def own_and_other(array):
        own = lax.dynamic_slice_in_dim(array, tp_index * half, half, 0)
        other = lax.dynamic_slice_in_dim(array, (1 - tp_index) * half, half, 0)
        return own, swap(other)

    ssm_own, ssm_other = own_and_other(ssm_out)
    joined = jnp.dot(ssm_own, out_ssm, preferred_element_type=jnp.float32) + jnp.dot(
        ssm_other, swapped_ssm, preferred_element_type=jnp.float32
    )
    stats, joined = lax.optimization_barrier((stats, joined))
    attn_out = attending.send(stats)
    attn_own, attn_other = own_and_other(attn_out)
    joined = joined + jnp.dot(attn_own, out_attn, preferred_element_type=jnp.float32)
    joined = joined + jnp.dot(attn_other, swapped_attn, preferred_element_type=jnp.float32)
    return joined.astype(jnp.bfloat16)


def solution(mesh):
    in_specs = (
        P(("fs", "sp"), "tp"),
        P(),
        P(None, "tp"),
        P(None, "tp"),
        P(None, "tp"),
        P(None, "tp"),
        P(None, "tp"),
        P(None, "tp"),
        P(None, "tp"),
        P(None, "tp"),
        P(None, "tp"),
        P(None, "tp"),
        P(None, "tp"),
        P("tp"),
        P(("fs", "sp"), "tp"),
        P("tp"),
        P(),
        P("tp"),
        P("tp", None),
        P("tp", None),
    )
    out_specs = P(("fs", "sp", "tp"), None)

    return jax.shard_map(
        per_device, mesh=mesh, in_specs=in_specs, out_specs=out_specs, check_vma=False
    )
```
